32 devices in a mesh: grp: 2 (over y), fs: 4 (over z), tp: 4 (over x, core).
Axes of the slice: x: 2, y: 2, z: 4, core: 2. Of those that a mesh axis runs over, the one named last changes fastest.
Arguments:
- tokens: bfloat16 [4096, 2048], P(('grp', 'fs'), 'tp'), parts along dimension 0, may hold values from -16 to 16
- attn_gain: float32 [2048], replicated, may hold values from 0.1 to 1.9
- w_query: bfloat16 [2048, 1024], P('fs', 'tp'), may hold values from -0.125 to 0.125
- w_key: bfloat16 [2048, 1024], P('fs', 'tp'), may hold values from -0.125 to 0.125
- w_value: bfloat16 [2048, 2048], P('fs', 'tp'), may hold values from -0.125 to 0.125
- w_low: bfloat16 [2048, 32], replicated, may hold values from -0.125 to 0.125
- w_lift: bfloat16 [32, 1024], P(None, 'tp'), may hold values from -1 to 1
- decay_bias: float32 [1024], P('tp'), may hold values from -0.5 to 6
- head_gain: float32 [256], replicated, may hold values from 0.1 to 1.9
- w_out: bfloat16 [2048, 2048], P('tp', 'fs'), may hold values from -0.125 to 0.125
- ffn_gain: float32 [2048], replicated, may hold values from 0.1 to 1.9
- w_gate: bfloat16 [2048, 5632], P('fs', 'tp'), may hold values from -0.125 to 0.125
- w_up: bfloat16 [2048, 5632], P('fs', 'tp'), may hold values from -0.125 to 0.125
- w_down: bfloat16 [5632, 2048], P('tp', 'fs'), may hold values from -0.078125 to 0.078125
- final_gain: float32 [2048], P('tp'), may hold values from 0.1 to 1.9
Outputs:
- result: bfloat16 [4096, 2048], P(('grp', 'fs'), 'tp'), parts along dimension 0
The draws below stay inside these ranges and needn't reach their ends.
There are 2 independent parts, one for each index of `grp`. The reference program is written for one: setup_inputs(seed, part) draws one part's arguments, and reference() takes and returns one part's arrays. A program takes and returns all parts, laid end to end along the dimension named above; an argument that names none is the same for every part. Nothing has to cross between parts.
All inputs are finite; a program needn't handle non-finite values.
Results may differ from the reference program's by a relative error of at most 0.015.
Values may be sent and summed in bfloat16 or wider, within the bound.
No kernel may reach another device: no remote copies, remote signals or barrier semaphores. Data moves between devices by JAX's collectives and lax.ppermute only.
A program may use at most 64 MiB of HBM per device.

```python
import math
import jax
import jax.numpy as jnp
from jax import lax

D = 2048
HEADS = 8
DK = 128
DV = 256
RANK = 32
FF = 5632
BLOCK = 64
LEN = 512
QK = 1024
V = 2048
TOKENS = 2048
N_FS = 4
N_TP = 4


def draw_tokens(key, part):
    first_key, second_key = jax.random.split(jax.random.fold_in(key, 11), 2)
    groups = 8
    scales = jnp.exp(jax.random.uniform(first_key, (groups,), jnp.float32, math.log(0.25), math.log(4.0)))
    scales = jnp.repeat(scales, D // groups)
    base = jnp.clip(jax.random.normal(second_key, (TOKENS, D), jnp.float32), -4.0, 4.0)
    return (base * scales[None, :]).astype(jnp.bfloat16)


def draw_decay_bias(key, part):
    first_key, second_key, third_key = jax.random.split(jax.random.fold_in(key, 23), 3)
    fast_share = 0.5
    is_fast = jax.random.uniform(first_key, (QK,), jnp.float32) < fast_share
    fast_value = jax.random.uniform(second_key, (QK,), jnp.float32, -0.5, 0.5)
    slow_value = jax.random.uniform(third_key, (QK,), jnp.float32, 4.5, 6.0)
    return jnp.where(is_fast, fast_value, slow_value)


def block_levels(stream_key, extent, shards, smallest, high):
    def one(axis_at, shards_of):
        heights = jax.random.uniform(jax.random.fold_in(jax.random.fold_in(stream_key, 6), axis_at), (shards_of,), jnp.float32, smallest / len(shards), high / len(shards))
        return jnp.repeat(jnp.exp(heights), extent[axis_at] // shards_of).reshape((-1,) + (1,) * (len(extent) - axis_at - 1))

    level = one(*shards[0])
    for cut in shards[1:]:
        level = level * one(*cut)
    return level


def noise(key, shape, width, bound, pieces=(), kind=jnp.bfloat16):
    values = width * jax.random.normal(key, shape, jnp.float32)
    if pieces:
        values = values * block_levels(key, shape, pieces, -0.22, 0.18)
    return jnp.clip(values, -bound, bound).astype(kind)


def setup_inputs(seed: int = 0, part: int = 0) -> dict:
    streams_of = jax.random.split(jax.random.key(seed), 16)
    own_keys = jax.random.split(jax.random.fold_in(streams_of[15], part), 16)
    return {
        "tokens": draw_tokens(jax.random.fold_in(jax.random.fold_in(streams_of[15], part), 71), part),
        "attn_gain": jnp.clip(1.0 + 0.18 * jax.random.normal(streams_of[1], (D,), jnp.float32), 0.1, 1.9),
        "w_query": noise(streams_of[2], (D, QK), D ** -0.5, 0.125, ((0, 4), (1, 4))),
        "w_key": noise(streams_of[3], (D, QK), D ** -0.5, 0.125, ((0, 4), (1, 4))),
        "w_value": noise(streams_of[4], (D, V), D ** -0.5, 0.125, ((0, 4), (1, 4))),
        "w_low": noise(streams_of[5], (D, RANK), D ** -0.5, 0.125),
        "w_lift": noise(streams_of[6], (RANK, QK), RANK ** -0.5, 1.0, ((1, 4),)),
        "decay_bias": draw_decay_bias(jax.random.fold_in(streams_of[15], 71), part),
        "head_gain": jnp.clip(1.0 + 0.18 * jax.random.normal(streams_of[8], (DV,), jnp.float32), 0.1, 1.9),
        "w_out": noise(streams_of[9], (V, D), V ** -0.5, 0.125, ((0, 4), (1, 4))),
        "ffn_gain": jnp.clip(1.0 + 0.18 * jax.random.normal(streams_of[10], (D,), jnp.float32), 0.1, 1.9),
        "w_gate": noise(streams_of[11], (D, FF), D ** -0.5, 0.125, ((0, 4), (1, 4))),
        "w_up": noise(streams_of[12], (D, FF), D ** -0.5, 0.125, ((0, 4), (1, 4))),
        "w_down": noise(streams_of[13], (FF, D), FF ** -0.5, 0.078125, ((0, 4), (1, 4))),
        "final_gain": jnp.clip(1.0 + 0.18 * jax.random.normal(streams_of[14], (D,), jnp.float32), 0.1, 1.9),
    }


epsilon = 1e-06
highest = lax.Precision.HIGHEST

def rms_rows(values, gain):
    values = values.astype(jnp.float32)
    factor = lax.rsqrt(lax.optimization_barrier(jnp.mean(values * values, axis=-1, keepdims=True)) + epsilon)
    return values * factor * gain.astype(jnp.float32)

def blockwise_gla(query_rows, key_rows, value_rows, log_decay, head_count):
    length = query_rows.shape[0]
    blocks = length // BLOCK

    def split_heads(array, depth):
        return array.astype(jnp.float32).reshape(blocks, BLOCK, head_count, depth).transpose(2, 0, 1, 3)
    query_f = split_heads(query_rows, DK) * DK ** (-0.5)
    key_f = split_heads(key_rows, DK)
    value_f = split_heads(value_rows, DV)
    log_cum = jnp.cumsum(split_heads(log_decay, DK), axis=2)
    log_last = log_cum[:, :, -1:, :]
    query_dec = query_f * jnp.exp(log_cum)
    key_dec = key_f * jnp.exp(-log_cum)
    causal = jnp.tril(jnp.ones((BLOCK, BLOCK), dtype=bool))
    scores = jnp.where(causal, jnp.einsum('hncd,hnsd->hncs', query_dec, key_dec, precision=highest), 0.0)
    inside = jnp.einsum('hncs,hnsv->hncv', scores, value_f, precision=highest)
    contrib = jnp.einsum('hncd,hncv->hndv', key_f * jnp.exp(log_last - log_cum), value_f, precision=highest)
    decay_block = jnp.exp(log_last[:, :, 0, :])

    def advance(carry_state, inputs):
        decay_step, added = inputs
        return (decay_step[..., None] * carry_state + added, carry_state)
    start_state = jnp.zeros((head_count, DK, DV), jnp.float32)
    final_state, earlier = lax.scan(advance, start_state, (jnp.moveaxis(decay_block, 1, 0), jnp.moveaxis(contrib, 1, 0)))
    earlier = jnp.moveaxis(earlier, 0, 1)
    output = inside + jnp.einsum('hncd,hndv->hncv', query_dec, earlier, precision=highest)
    return output.transpose(1, 2, 0, 3).reshape(length, head_count, DV)

def reference(tokens, attn_gain, w_query, w_key, w_value, w_low, w_lift, decay_bias, head_gain, w_out, ffn_gain, w_gate, w_up, w_down, final_gain):
    normed = rms_rows(tokens, attn_gain).astype(jnp.bfloat16)
    query_rows = jnp.dot(normed, w_query, preferred_element_type=jnp.float32).astype(jnp.bfloat16)
    key_rows = jnp.dot(normed, w_key, preferred_element_type=jnp.float32).astype(jnp.bfloat16)
    value_rows = jnp.dot(normed, w_value, preferred_element_type=jnp.float32).astype(jnp.bfloat16)
    low_rank = jnp.dot(normed, w_low, preferred_element_type=jnp.float32).astype(jnp.bfloat16)
    log_decay = jax.nn.log_sigmoid(jnp.dot(low_rank, w_lift, preferred_element_type=jnp.float32) + decay_bias.astype(jnp.float32)) / 16.0
    gla_out = jax.vmap(lambda qq, kk, vv, gg: blockwise_gla(qq, kk, vv, gg, HEADS))(query_rows.reshape(N_FS, LEN, QK), key_rows.reshape(N_FS, LEN, QK), value_rows.reshape(N_FS, LEN, V), log_decay.reshape(N_FS, LEN, QK))
    gla_out = gla_out.reshape(TOKENS, HEADS, DV)
    mixed_heads = rms_rows(gla_out, head_gain).reshape(TOKENS, V).astype(jnp.bfloat16)
    span = V // N_TP
    attn_sum = jnp.zeros((TOKENS, D), jnp.float32)
    for index in range(N_TP):
        partial_prod = jnp.dot(mixed_heads[:, index * span:(index + 1) * span], w_out[index * span:(index + 1) * span], preferred_element_type=jnp.float32).astype(jnp.bfloat16)
        attn_sum = attn_sum + partial_prod.astype(jnp.float32)
    first_sum = (tokens.astype(jnp.float32) + attn_sum).astype(jnp.bfloat16)
    normed_ffn = rms_rows(first_sum, ffn_gain).astype(jnp.bfloat16)
    gate_rows = jnp.dot(normed_ffn, w_gate, preferred_element_type=jnp.float32)
    up_rows = jnp.dot(normed_ffn, w_up, preferred_element_type=jnp.float32)
    hidden = (jax.nn.silu(gate_rows) * up_rows).astype(jnp.bfloat16)
    units = FF // N_TP
    ffn_sum = jnp.zeros((TOKENS, D), jnp.float32)
    for index in range(N_TP):
        partial_prod = jnp.dot(hidden[:, index * units:(index + 1) * units], w_down[index * units:(index + 1) * units], preferred_element_type=jnp.float32).astype(jnp.bfloat16)
        ffn_sum = ffn_sum + partial_prod.astype(jnp.float32)
    second_sum = first_sum.astype(jnp.float32) + ffn_sum
    return rms_rows(second_sum, final_gain).astype(jnp.bfloat16)
```

```python
import functools

import jax
import jax.numpy as jnp
from jax import lax
from jax.experimental import pallas as pl
from jax.experimental.pallas import tpu as pltpu
from jax.sharding import PartitionSpec as P

DK = 128
DV = 256
BLOCK = 64

epsilon = 1e-06
bf16 = jnp.bfloat16
f32 = jnp.float32


def mixer_kernel(heads, q_ref, k_ref, v_ref, low_ref, lift_ref, bias_ref, gain_ref, out_ref):
    length = q_ref.shape[0]
    row = lax.broadcasted_iota(jnp.int32, (BLOCK, BLOCK), 0)
    col = lax.broadcasted_iota(jnp.int32, (BLOCK, BLOCK), 1)
    causal = row >= col
    ones = causal.astype(f32)
    logits = jnp.dot(low_ref[...], lift_ref[...], preferred_element_type=f32) + bias_ref[...]
    decay = (jnp.minimum(logits, 0.0) - jnp.log1p(jnp.exp(-jnp.abs(logits)))) / 16.0
    states = [jnp.zeros((DK, DV), f32) for _ in range(heads)]
    for block in range(length // BLOCK):
        rows = slice(block * BLOCK, (block + 1) * BLOCK)
        cum = jnp.dot(
            ones, decay[rows], preferred_element_type=f32, precision=lax.Precision.HIGHEST
        )
        last = cum[BLOCK - 1 : BLOCK]
        grow = jnp.exp(cum)
        key = k_ref[rows, :].astype(f32)
        query_dec = (q_ref[rows, :].astype(f32) * (DK**-0.5) * grow).astype(bf16)
        key_dec = (key * jnp.exp(-cum)).astype(bf16)
        key_end = (key * jnp.exp(last - cum)).astype(bf16)
        step = jnp.exp(last)
        for head in range(heads):
            chan = slice(head * DK, (head + 1) * DK)
            vals = slice(head * DV, (head + 1) * DV)
            value = v_ref[rows, vals]
            scores = lax.dot_general(
                query_dec[:, chan],
                key_dec[:, chan],
                (((1,), (1,)), ((), ())),
                preferred_element_type=f32,
            )
            scores = jnp.where(causal, scores, 0.0).astype(bf16)
            out = jnp.dot(scores, value, preferred_element_type=f32)
            out += jnp.dot(
                query_dec[:, chan], states[head].astype(bf16), preferred_element_type=f32
            )
            added = lax.dot_general(
                key_end[:, chan], value, (((0,), (0,)), ((), ())), preferred_element_type=f32
            )
            states[head] = jnp.transpose(step[:, chan]) * states[head] + added
            factor = lax.rsqrt(jnp.mean(out * out, axis=-1, keepdims=True) + epsilon)
            out_ref[rows, vals] = (out * factor * gain_ref[...]).astype(bf16)


def mixer(query, key, value, low, lift, bias, gain):
    heads = query.shape[1] // DK
    spec = pl.BlockSpec(memory_space=pltpu.VMEM)
    return pl.pallas_call(
        functools.partial(mixer_kernel, heads),
        out_shape=jax.ShapeDtypeStruct(value.shape, bf16),
        in_specs=[spec] * 7,
        out_specs=spec,
        cost_estimate=pl.CostEstimate(
            flops=10_000_000_000, bytes_accessed=4_000_000, transcendentals=1_000_000
        ),
        name="mixer",
    )(query, key, value, low, lift, bias.reshape(1, -1), gain.reshape(1, -1))


def body(sizes, tokens, attn_gain, w_query, w_key, w_value, w_low, w_lift, decay_bias,
         head_gain, w_out, ffn_gain, w_gate, w_up, w_down, final_gain):
    n_grp, n_fs, n_tp = sizes
    rows, width = tokens.shape
    features = width * n_tp
    unit = features // (n_fs * n_grp)
    grp, fs, tp = (lax.axis_index(name) for name in ("grp", "fs", "tp"))

    def send(value, axis, pairs):
        return lax.ppermute(value, axis, pairs)

    def line(part):
        if n_fs == 4:
            near = send(part, "fs", [(0, 1), (1, 0), (2, 3), (3, 2)])
            first = send(part, "fs", [(1, 2), (2, 1)])
            second = send(near, "fs", [(1, 2), (2, 1)])
            first = first + send(first, "fs", [(1, 0), (2, 3)])
            second = second + send(second, "fs", [(1, 0), (2, 3)])
            return [near, first, second]
        right, left, rights, lefts = part, part, [], []
        for step in range(1, n_fs):
            right = send(right, "fs", [(i, i + 1) for i in range(step - 1, n_fs - 1)])
            left = send(left, "fs", [(i + 1, i) for i in range(n_fs - step)])
            rights.append(right)
            lefts.append(left)
        return [rights[s] + lefts[n_fs - 2 - s] for s in range(n_fs - 1)]

    if n_fs == 4:
        owners = [fs ^ 1, jnp.where(fs < 2, 2, 1), jnp.where(fs < 2, 3, 0)]
    else:
        owners = [(fs + n_fs - s) % n_fs for s in range(1, n_fs)]
    order = [fs * n_grp + i for i in range(n_grp)]
    for owner in owners:
        order += [owner * n_grp + (grp + k) % n_grp for k in range(n_grp)]

    def gather(shard, axis):
        size = shard.shape[axis] // n_grp
        part = lax.dynamic_slice_in_dim(shard, grp * size, size, axis)
        parts = [lax.slice_in_dim(shard, i * size, (i + 1) * size, axis=axis) for i in range(n_grp)]
        for got in line(part):
            parts.append(got)
            for k in range(1, n_grp):
                parts.append(send(got, "grp", [((i + k) % n_grp, i) for i in range(n_grp)]))
        return jnp.concatenate(parts, axis=axis)

    bits = [1 << i for i in range(n_tp.bit_length() - 1)]

    def flip(value, bit):
        return send(value, "tp", [(i, i ^ bit) for i in range(n_tp)])

    def gather_tp(own):
        held = own[None]
        for bit in reversed(bits):
            held = jnp.concatenate([held, flip(held, bit)], 0)
        index = [0]
        for bit in reversed(bits):
            index += [i ^ bit for i in index]
        return [held[index.index(r)] for r in range(n_tp)]

    def scatter_tp(blocks):
        owners_left = [0]
        have = {r: blocks(tp ^ r) for r in range(n_tp)}
        for bit in bits:
            keep = [r for r in have if not r & bit]
            sent = jnp.stack([have[r | bit] for r in keep])
            got = flip(sent, bit)
            have = {
                r: (have[r].astype(f32) + got[i].astype(f32)).astype(bf16 if bit != bits[-1] else f32)
                for i, r in enumerate(keep)
            }
        return have[0]

    per_tp = width // unit

    def norm_permuted(pieces, gain):
        squares = sum(
            jnp.sum(jnp.square(piece.astype(f32)), axis=1, keepdims=True) for piece in pieces
        )
        factor = lax.rsqrt(squares / features + epsilon)
        stack = jnp.stack(
            [piece[:, i * unit : (i + 1) * unit] for piece in pieces for i in range(per_tp)]
        )
        gains = gain.reshape(-1, 1, unit)
        parts = []
        for at in order:
            place = ((at // per_tp) ^ tp) * per_tp + at % per_tp
            part = lax.dynamic_index_in_dim(stack, place, 0, keepdims=False).astype(f32)
            scale = lax.dynamic_index_in_dim(gains, at, 0, keepdims=False)
            parts.append((part * factor * scale).astype(bf16))
        return jnp.concatenate(parts, axis=1)

    def dot(a, b):
        return jnp.dot(a, b, preferred_element_type=f32)

    def position(at):
        place = 0
        for i, value in enumerate(order):
            place = place + jnp.where(value == at, i, 0)
        return place

    places = [position(at) for at in range(n_fs * n_grp)]
    place_of = jnp.stack(places)

    def owner_blocks(terms):
        stack = jnp.stack([terms[:, i * unit : (i + 1) * unit] for i in range(len(order))])

        def block(owner):
            return jnp.concatenate(
                [
                    lax.dynamic_index_in_dim(stack, place_of[owner * per_tp + i], 0, keepdims=False)
                    for i in range(per_tp)
                ],
                axis=1,
            )

        return block

    mix_weights = gather(jnp.concatenate([w_query, w_key, w_value], axis=1), 0)
    out_weights = gather(w_out, 1)
    gate_weights = gather(w_gate, 0)
    up_weights = gather(w_up, 0)
    down_weights = gather(w_down, 1)

    normed = norm_permuted(gather_tp(tokens), attn_gain)
    mixed_in = dot(normed, mix_weights).astype(bf16)
    keys = w_query.shape[1]
    low_order = jnp.concatenate(
        [lax.dynamic_slice_in_dim(w_low, at * unit, unit, 0) for at in order], 0
    )
    low = dot(normed, low_order).astype(bf16)
    mixed = mixer(
        mixed_in[:, :keys], mixed_in[:, keys : 2 * keys], mixed_in[:, 2 * keys :],
        low, w_lift, decay_bias, head_gain,
    )
    out_terms = dot(mixed, out_weights).astype(bf16)
    attn = scatter_tp(owner_blocks(out_terms))
    first_sum = (tokens.astype(f32) + attn).astype(bf16)
    normed_ffn = norm_permuted(gather_tp(first_sum), ffn_gain)
    gate_rows = dot(normed_ffn, gate_weights)
    up_rows = dot(normed_ffn, up_weights)
    hidden = (jax.nn.silu(gate_rows) * up_rows).astype(bf16)
    down_terms = dot(hidden, down_weights).astype(bf16)
    second_sum = first_sum.astype(f32) + scatter_tp(owner_blocks(down_terms))
    squares = jnp.sum(second_sum * second_sum, axis=1)
    for bit in bits:
        squares = squares + flip(squares, bit)
    factor = lax.rsqrt(squares / features + epsilon)[:, None]
    return (second_sum * factor * final_gain).astype(bf16)


def solution(mesh):
    sizes = tuple(mesh.shape[name] for name in ("grp", "fs", "tp"))
    return jax.shard_map(
        functools.partial(body, sizes),
        mesh=mesh,
        in_specs=(
            P(("grp", "fs"), "tp"),
            P(),
            P("fs", "tp"),
            P("fs", "tp"),
            P("fs", "tp"),
            P(),
            P(None, "tp"),
            P("tp"),
            P(),
            P("tp", "fs"),
            P(),
            P("fs", "tp"),
            P("fs", "tp"),
            P("tp", "fs"),
            P("tp"),
        ),
        out_specs=P(("grp", "fs"), "tp"),
        check_vma=False,
    )
```
